32 devices in a mesh: sp: 8 (over z, core), tp: 4 (over y, x).
Axes of the slice: x: 2, y: 2, z: 4, core: 2. Of those that a mesh axis runs over, the one named last changes fastest.
Arguments:
- outer_gate: bfloat16 [2048, 1024], P('sp', 'tp'), may hold values from -6 to 6
- inner_gate: bfloat16 [2048, 1024], P('sp', 'tp'), may hold values from -6 to 6
- values: bfloat16 [2048, 1024], P('sp', 'tp'), may hold values from -6 to 6
- conv_taps: bfloat16 [3, 1024], P(None, 'tp'), may hold values from -3.5 to 3.5
- document: int32 [2048], P('sp'), may hold values from 0 to 3, never falling along the last dimension, each value on 1 to 1024 neighbouring positions
- mix_proj: bfloat16 [1024, 2048], P('tp'), may hold values from -0.1875 to 0.1875
- stream: bfloat16 [2048, 2048], P('sp'), may hold values from -6 to 6
- norm_gain: float32 [2048], replicated, may hold values from 0.1 to 1.9
- routes: int32 [2048, 2], P('sp'), may hold values from 0 to 7, all different within a row; in each aligned block of 256 rows (0 to 255, 256 to 511, ...) at most 96 rows name the same one
- route_weight: float32 [2048, 2], P('sp'), may hold values from 0.25 to 1
- w_gate: bfloat16 [8, 2048, 4096], P('sp', None, 'tp'), may hold values from -0.125 to 0.125
- w_up: bfloat16 [8, 2048, 4096], P('sp', None, 'tp'), may hold values from -0.125 to 0.125
- w_down: bfloat16 [8, 4096, 2048], P('sp', 'tp'), may hold values from -0.09375 to 0.09375
Outputs:
- mixed: bfloat16 [2048, 2048], P('sp', 'tp')
The draws below stay inside these ranges and needn't reach their ends.
Inputs may be any that keep to these rules, and one draw needn't show every extreme that they name: Document numbers never fall along the sequence; each document holds 1 to 1024 consecutive tokens and one holds exactly that many. `routes`: each token names 2 different experts. Among the 256 tokens of one sp index no expert is named by more than 96 tokens, and in some sp index's tokens an expert is named by exactly 96.
All inputs are finite; a program needn't handle non-finite values.
Results may differ from the reference program's by a relative error of at most 0.014.
Values may be sent and summed in bfloat16 or wider, within the bound.
A program may use at most 64 MiB of HBM per device.

```python
import math
import jax
import jax.numpy as jnp
import numpy as np
from jax import lax

D = 2048
DC = 1024
FFE = 4096
TOP = 2
TAPS = 3
T_SP = 256
TOKENS = 2048
EXPERTS = 8
CAP = 96
N_SP = 8
N_TP = 4


def shard_levels(stream_key, shape, shards, smallest, high):
    gain, own = 1.0, jax.random.fold_in(stream_key, 6)
    for dim, shards_of in shards:
        heights = jnp.exp(jax.random.uniform(jax.random.fold_in(own, dim), (shards_of,), jnp.float32, smallest / len(shards), high / len(shards)))
        gain = gain * jnp.repeat(heights, shape[dim] // shards_of).reshape([-1 if axis == dim else 1 for axis in range(len(shape))])
    return gain


def split_up(amount, total, most, slope):
    weights = [(1 << 20) // math.isqrt(standing ** slope) + 1 for standing in range(2, amount + 1)]
    spare, holding = total - most - (amount - 1), [1] * (amount - 1)
    while spare > 0:
        free = [i for i in range(amount - 1) if holding[i] < most]
        pool, remaining = sum([weights[i] for i in free]), spare
        for i in free:
            extra = min(most - holding[i], max(1, remaining * weights[i] // pool), spare)
            holding[i] = holding[i] + extra
            spare = spare - extra
    return np.array([most] + holding)


def ragged(stream_key, number_of, total, most, slope):
    if number_of == 2:
        one = jax.random.randint(stream_key, (), max(1, total - most), min(most, total - 1) + 1)
        return jnp.stack([one, total - one])
    lengths = jnp.asarray(split_up(number_of, total, most, slope), jnp.int32)
    pairs = (number_of - 1) // 2
    source_of, sink = lengths[1:1 + 2 * pairs:2], lengths[2:2 + 2 * pairs:2]
    slack = jnp.minimum(source_of - 1, most - sink)
    moved = jax.random.randint(jax.random.fold_in(stream_key, 1), (pairs,), 0, 1 << 20) % (slack + 1)
    lengths = lengths.at[1:1 + 2 * pairs:2].set(source_of - moved).at[2:2 + 2 * pairs:2].set(sink + moved)
    return lengths[jax.random.permutation(jax.random.fold_in(stream_key, 2), number_of)]


def assign_block(stream_key, own, number, rows, count, top, most, slope):
    ranking = jax.random.permutation(stream_key, count)
    packed, usual = load_shares(count, rows * top, most, slope, True), load_shares(count, rows * top, most, slope, False)
    places = jnp.arange(count)

    def named(lengths, turn):
        used = int((lengths > 0).sum())
        fixed = max(1, used // 4)
        moved = fixed + (places - fixed + turn * (used - fixed)) % max(1, count - fixed)
        return jnp.zeros((count,), jnp.int32).at[ranking[jnp.where(places < fixed, places, moved)]].set(jnp.asarray(lengths, jnp.int32))

    lengths = jnp.where(number % 4 == 0, named(packed, number // 4), named(usual, number - number // 4 - 1))
    mixed = jax.random.permutation(jax.random.fold_in(own, 3), count)
    source_of, taker = mixed[0:count // 2 * 2:2], mixed[1:count // 2 * 2:2]
    margin = jnp.minimum(lengths[source_of] - 1, most - lengths[taker]) // 2
    margin = jnp.where((source_of == ranking[0]) | (taker == ranking[0]) | (lengths[taker] == 0), 0, jnp.maximum(margin, 0))
    moved = jax.random.randint(jax.random.fold_in(own, 4), (count // 2,), 0, 1 << 20) % (margin + 1)
    lengths = lengths.at[source_of].add(-moved).at[taker].add(moved)
    items = jnp.searchsorted(jnp.cumsum(lengths), jnp.arange(rows * top), side="right").astype(jnp.int32)
    listing = items.reshape(top, rows).T
    listing = listing[jax.random.permutation(jax.random.fold_in(own, 1), rows)]
    turn = jax.random.randint(jax.random.fold_in(own, 2), (rows, 1), 0, top)
    return jnp.take_along_axis(listing, (jnp.arange(top)[None, :] + turn) % top, axis=1)


def load_shares(amount, total, bound, lean, full):
    weights = [(1 << 20) // math.isqrt(rank ** lean) + 1 for rank in range(1, amount + 1)]
    largest = bound if full else min(bound, max(-(-total // amount), total * weights[0] // sum(weights)))
    least = 1 if total - largest >= amount - 1 else 0
    counts, rest = [largest] + [least] * (amount - 1), total - largest - least * (amount - 1)
    while rest > 0:
        candidates = [i for i in range(1, amount) if counts[i] < largest] or [i for i in range(1, amount) if counts[i] < bound]
        pool, budget = sum([weights[i] for i in candidates]), rest
        for i in candidates:
            extra = min(bound - counts[i], max(1, budget * weights[i] // pool), rest)
            counts[i] = counts[i] + extra
            rest = rest - extra
    return np.array(counts)


def centred(stream_key, extent, deviation, reach, cuts=(), kind=jnp.bfloat16):
    factor_of = shard_levels(stream_key, extent, cuts, -0.22, 0.18) if cuts else 1.0
    drawn = jax.random.normal(stream_key, extent, jnp.float32) * deviation * factor_of
    return jnp.minimum(jnp.maximum(drawn, -reach), reach).astype(kind)


def setup_inputs(seed: int = 0) -> dict:
    key_list = jax.random.split(jax.random.key(seed), 14)
    outer_gate = centred(key_list[0], (TOKENS, DC), 1.0, 6.0, ((0, 8), (1, 4)))
    inner_gate = centred(key_list[1], (TOKENS, DC), 1.0, 6.0, ((0, 8), (1, 4)))
    values = centred(key_list[2], (TOKENS, DC), 1.0, 6.0, ((0, 8), (1, 4)))
    conv_taps = centred(key_list[3], (TAPS, DC), TAPS ** -0.5, 3.5, ((1, 4),))
    document = jnp.searchsorted(jnp.cumsum(ragged(key_list[4], N_SP // 2, TOKENS, 4 * T_SP, 1)), jnp.arange(TOKENS), side="right").astype(jnp.int32)
    mix_proj = centred(key_list[5], (DC, D), DC ** -0.5, 0.1875, ((0, 4),))
    stream = centred(key_list[6], (TOKENS, D), 1.0, 6.0, ((0, 8),))
    norm_gain = jnp.clip(1.0 + 0.18 * jax.random.normal(key_list[7], (D,), jnp.float32), 0.1, 1.9)
    routes_keys = jax.random.split(jax.random.fold_in(key_list[8], 1), TOKENS // T_SP)
    routes_turns = jax.random.permutation(jax.random.fold_in(key_list[8], 3), TOKENS // T_SP)
    routes = jax.vmap(lambda own, number: assign_block(jax.random.fold_in(key_list[8], 2), own, number, T_SP, EXPERTS, TOP, CAP, 2))(routes_keys, routes_turns).reshape((TOKENS, TOP))
    route_weight = jnp.clip(0.25 + 0.75 * jax.random.uniform(key_list[9], (TOKENS, TOP), jnp.float32) ** shard_levels(key_list[9], (TOKENS, TOP), ((0, 8),), -0.2, 0.2), 0.25, 1.0)
    w_gate = centred(key_list[10], (EXPERTS, D, FFE), D ** -0.5, 0.125, ((0, 8), (2, 4)))
    w_up = centred(key_list[11], (EXPERTS, D, FFE), D ** -0.5, 0.125, ((0, 8), (2, 4)))
    w_down = centred(key_list[12], (EXPERTS, FFE, D), FFE ** -0.5, 0.09375, ((0, 8), (1, 4)))
    return {"outer_gate": outer_gate, "inner_gate": inner_gate, "values": values, "conv_taps": conv_taps, "document": document, "mix_proj": mix_proj, "stream": stream, "norm_gain": norm_gain, "routes": routes, "route_weight": route_weight, "w_gate": w_gate, "w_up": w_up, "w_down": w_down}


def rounded(value):
    held = lax.optimization_barrier(value.astype(jnp.bfloat16))
    return held.astype(jnp.float32)

def reference(outer_gate, inner_gate, values, conv_taps, document, mix_proj, stream, norm_gain, routes, route_weight, w_gate, w_up, w_down):
    length = stream.shape[0]
    product = inner_gate.astype(jnp.float32) * values.astype(jnp.float32)
    kernel = conv_taps.astype(jnp.float32)
    conv = kernel[2] * product
    for back in (1, 2):
        shifted = jnp.pad(product, ((back, 0), (0, 0)))[:length]
        earlier = jnp.pad(document, (back, 0), constant_values=-1)[:length]
        same = (earlier == document)[:, None]
        conv = conv + kernel[2 - back] * jnp.where(same, shifted, 0.0)
    gated = (outer_gate.astype(jnp.float32) * conv).astype(jnp.bfloat16)
    group_width = DC // N_TP
    branch = jnp.zeros((length, D), jnp.float32)
    for group in range(N_TP):
        lower = group * group_width
        partial_value = jnp.dot(gated[:, lower:lower + group_width], mix_proj[lower:lower + group_width], preferred_element_type=jnp.float32)
        branch = branch + rounded(partial_value)
    hidden_state = stream.astype(jnp.float32) + branch
    scale = lax.rsqrt(lax.optimization_barrier(jnp.mean(hidden_state * hidden_state, axis=-1, keepdims=True)) + 1e-06)
    normed = (hidden_state * scale * norm_gain).astype(jnp.bfloat16)
    flat_expert = routes.reshape(-1).astype(jnp.int32)
    count = flat_expert.shape[0]
    flat_token = jnp.arange(count, dtype=jnp.int32) // TOP
    flat_weight = route_weight.reshape(-1)
    order_key = jnp.arange(count, dtype=jnp.int32)
    limit = N_SP * CAP
    hidden_width = FFE // N_TP

    def per_expert(carry, expert):
        keyed = jnp.where(flat_expert == expert, order_key, count)
        chosen = jnp.argsort(keyed, stable=True)[:limit].astype(jnp.int32)
        valid = jnp.take(keyed, chosen) < count
        token_index = jnp.take(flat_token, chosen)
        taken = jnp.take(normed, token_index, axis=0)
        gate = jnp.dot(taken, w_gate[expert], preferred_element_type=jnp.float32)
        upper = jnp.dot(taken, w_up[expert], preferred_element_type=jnp.float32)
        act = (jax.nn.silu(gate) * upper).astype(jnp.bfloat16)
        down = w_down[expert]
        total = jnp.zeros((limit, D), jnp.float32)
        for group in range(N_TP):
            lower = group * hidden_width
            partial_value = jnp.dot(act[:, lower:lower + hidden_width], down[lower:lower + hidden_width], preferred_element_type=jnp.float32)
            total = total + rounded(partial_value)
        expert_out = rounded(total)
        weight = jnp.where(valid, jnp.take(flat_weight, chosen), 0.0)
        carry = carry.at[token_index].add(weight[:, None] * expert_out)
        return (carry, None)
    combined, _ = lax.scan(per_expert, jnp.zeros((length, D), jnp.float32), jnp.arange(EXPERTS, dtype=jnp.int32))
    return (hidden_state + combined).astype(jnp.bfloat16)
```

```python
import functools

import jax
import jax.numpy as jnp
from jax import lax
from jax.experimental import pallas as pl
from jax.experimental.pallas import tpu as pltpu
from jax.sharding import PartitionSpec as P

F32 = jnp.float32
BF16 = jnp.bfloat16
MESH = pl.DeviceIdType.MESH
GROUP = 2


def xor(value, mask, count):
    out, bit = value, 1
    while bit < count:
        if isinstance(mask, int):
            if mask & bit:
                out = out + bit * (1 - 2 * lax.rem(lax.div(value, bit), 2))
        else:
            ours = lax.rem(lax.div(value, bit), 2)
            other = lax.rem(lax.div(mask, bit), 2)
            out = out + bit * other * (1 - 2 * ours)
        bit *= 2
    return out


def kernel(
    n_sp, n_tp, cap,
    outer, inner, vals, taps, doc, routes_c, routes_r, rw, gain,
    mix_hbm, stream_hbm, wg_hbm, wu_hbm, wd_hbm,
    out,
    mix, own, wg, wu, wd, rim_out, rim_in, prod_pad, doc_pad,
    bpart, brecv, hidden, obuf, xbuf, pbuf, r1, act, ret, back, acc,
    local_sem, rim_s, rim_r, br_s, br_r, z_s, z_r, ag_s, ag_r, rs_s, rs_r, bk_s, bk_r,
):
    s, p = lax.axis_index("sp"), lax.axis_index("tp")
    length, channels = outer.shape
    width = own.shape[1]
    features = mix.shape[1]
    hidden_units = wg.shape[1]
    x_side = 1
    while x_side * x_side < n_tp:
        x_side *= 2
    x_set = list(range(x_side))
    y_set = [k * x_side for k in range(n_tp // x_side)]

    def at(index):
        return pl.multiple_of(index * width, width)

    loads = [
        pltpu.make_async_copy(mix_hbm, mix, local_sem.at[0]),
        pltpu.make_async_copy(stream_hbm.at[:, pl.ds(at(p), width)], own, local_sem.at[1]),
        pltpu.make_async_copy(wg_hbm.at[0], wg, local_sem.at[2]),
        pltpu.make_async_copy(wu_hbm.at[0], wu, local_sem.at[3]),
        pltpu.make_async_copy(wd_hbm.at[0], wd, local_sem.at[4]),
    ]
    for load in loads:
        load.start()

    barrier = pltpu.get_barrier_semaphore()
    for d in range(1, n_sp):
        pl.semaphore_signal(barrier, inc=1, device_id={"sp": xor(s, d, n_sp)}, device_id_type=MESH)
    for r in range(1, n_tp):
        pl.semaphore_signal(barrier, inc=1, device_id={"tp": xor(p, r, n_tp)}, device_id_type=MESH)
    product = inner[...].astype(F32) * vals[...].astype(F32)
    prod_pad[8:, :] = product
    docs = jnp.broadcast_to(doc[...], (length, channels))
    doc_pad[8:, :] = docs
    rim_out[:8, :] = product[length - 8 :]
    rim_out[8:, :] = docs[length - 8 :]
    pl.semaphore_wait(barrier, n_sp - 1 + n_tp - 1)

    sends = []

    def send(src, dst, s_sem, r_sem, **device):
        copy = pltpu.make_async_remote_copy(
            src_ref=src, dst_ref=dst, send_sem=s_sem, recv_sem=r_sem,
            device_id=device, device_id_type=MESH,
        )
        copy.start()
        sends.append(copy)
        return copy

    rim = send(rim_out, rim_in, rim_s, rim_r, sp=lax.rem(s + 1, n_sp))

    row = lax.broadcasted_iota(jnp.int32, (length, length), 0)
    col = lax.broadcasted_iota(jnp.int32, (length, length), 1)
    expert_r = lax.broadcasted_iota(jnp.int32, (max(n_sp, 16), length), 0)
    in_r = ((routes_r[0:1, :] == expert_r) | (routes_r[1:2, :] == expert_r)).astype(F32)
    rank_r = jnp.dot(in_r.astype(BF16), (row < col).astype(F32).astype(BF16), preferred_element_type=F32)
    expert_c = lax.broadcasted_iota(jnp.int32, (length, 128), 1)
    in_c = ((routes_c[:, 0:1] == expert_c) | (routes_c[:, 1:2] == expert_c)).astype(F32)
    rank_c = jnp.dot((row > col).astype(F32).astype(BF16), in_c.astype(BF16), preferred_element_type=F32)
    rank_r = jnp.where(in_r > 0, rank_r, -1.0)
    rank_c = jnp.where(in_c > 0, rank_c, -1.0)

    loads[0].wait()
    rim.wait_recv()
    prod_pad[:8, :] = rim_in[:8, :]
    doc_pad[:8, :] = jnp.where(s > 0, rim_in[8:, :], -1.0)
    kernel_taps = taps[...].astype(F32)
    conv = kernel_taps[2:3] * product
    for step in (1, 2):
        same = doc_pad[pl.ds(8 - step, length), :] == docs
        conv = conv + kernel_taps[2 - step : 3 - step] * jnp.where(same, prod_pad[pl.ds(8 - step, length), :], 0.0)
    gated = (outer[...].astype(F32) * conv).astype(BF16)
    for r in list(range(n_tp - 1, 0, -1)) + [0]:
        q = xor(p, r, n_tp)
        bpart[r] = jnp.dot(gated, mix[:, pl.ds(at(q), width)], preferred_element_type=F32).astype(BF16)
        if r:
            send(bpart.at[r], brecv.at[r], br_s.at[r], br_r.at[r], tp=q)
    loads[1].wait()
    total = bpart[0].astype(F32)
    for r in range(1, n_tp):
        pltpu.make_async_copy(brecv.at[r], brecv.at[r], br_r.at[r]).wait()
        total = total + brecv[r].astype(F32)
    total = total + own[...].astype(F32)
    hidden[...] = total
    scaled = (total * gain[pl.ds(p, 1), :]).astype(BF16)

    slot_r = lax.broadcasted_iota(jnp.int32, (cap, length), 0).astype(F32)
    for d in list(range(n_sp)):
        e = xor(s, d, n_sp)
        line = jnp.sum(jnp.where(expert_r == e, rank_r, 0.0), axis=0, keepdims=True)
        pick = (line == slot_r).astype(F32).astype(BF16)
        rows = jnp.dot(pick, scaled, preferred_element_type=F32).astype(BF16)
        if d == 0:
            xbuf[0, 0] = rows
        else:
            obuf[d] = rows
            send(obuf.at[d], xbuf.at[0, d], z_s.at[d], z_r.at[d], sp=e)

    def arrived(ref, sem):
        pltpu.make_async_copy(ref, ref, sem).wait()

    def axes(d):
        return (x_set, y_set) if d % 2 == 0 else (y_set, x_set)

    def gather_first(d):
        first, _ = axes(d)
        if d:
            arrived(xbuf.at[0, d], z_r.at[d])
        for f in first[1:]:
            send(xbuf.at[0, d], xbuf.at[f, d], ag_s.at[d, f], ag_r.at[d, f], tp=xor(p, f, n_tp))

    def gather_second(d):
        first, second = axes(d)
        for f in first:
            if f:
                arrived(xbuf.at[f, d], ag_r.at[d, f])
            for g in second[1:]:
                send(
                    xbuf.at[f, d], xbuf.at[f + g, d], ag_s.at[d, f + g], ag_r.at[d, f + g],
                    tp=xor(p, g, n_tp),
                )

    tile = min(256, hidden_units)

    def expert(step):
        low = step * GROUP
        for d in range(low, low + GROUP):
            first, second = axes(d)
            for f in first:
                for g in second[1:]:
                    arrived(xbuf.at[f + g, d], ag_r.at[d, f + g])
        square = jnp.zeros((GROUP * cap, 1), F32)
        for r in range(n_tp):
            inverse = 1.0 / gain[pl.ds(xor(p, r, n_tp), 1), :]
            plain = xbuf[r, low : low + GROUP].reshape(GROUP * cap, width).astype(F32) * inverse
            square = square + jnp.sum(plain * plain, axis=1, keepdims=True)
        scale = lax.rsqrt(square / features + 1e-06)

        def up_tile(j, _):
            lanes = pl.ds(pl.multiple_of(j * tile, tile), tile)
            gate = jnp.zeros((GROUP * cap, tile), F32)
            upper = jnp.zeros((GROUP * cap, tile), F32)
            for r in range(n_tp):
                lhs = xbuf[r, low : low + GROUP].reshape(GROUP * cap, width)
                deep = pl.ds(at(xor(p, r, n_tp)), width)
                gate = gate + jnp.dot(lhs, wg[deep, lanes], preferred_element_type=F32)
                upper = upper + jnp.dot(lhs, wu[deep, lanes], preferred_element_type=F32)
            gate, upper = gate * scale, upper * scale
            act[:, lanes] = (gate / (1.0 + jnp.exp(-gate)) * upper).astype(BF16)
            return 0

        lax.fori_loop(0, hidden_units // tile, up_tile, 0)

        def down_tile(r, _):
            lanes = pl.ds(at(xor(p, r, n_tp)), width)
            part = jnp.dot(act[...], wd[:, lanes], preferred_element_type=F32).astype(BF16)
            pbuf[r, low : low + GROUP] = part.reshape(GROUP, cap, width)
            return 0

        lax.fori_loop(0, n_tp, down_tile, 0)
        for d in range(low, low + GROUP):
            first, second = axes(d)
            for f in first[1:]:
                for g in second[::-1]:
                    send(
                        pbuf.at[f + g, d], r1.at[f + g, d], rs_s.at[d, f + g], rs_r.at[d, f + g],
                        tp=xor(p, f, n_tp),
                    )

    def scatter_second(d):
        first, second = axes(d)
        for g in second[1:]:
            part = pbuf[g, d].astype(F32)
            for f in first[1:]:
                arrived(r1.at[f + g, d], rs_r.at[d, f + g])
                part = part + r1[f + g, d].astype(F32)
            pbuf[g, d] = part.astype(BF16)
            send(pbuf.at[g, d], r1.at[g, d], rs_s.at[d, g], rs_r.at[d, g], tp=xor(p, g, n_tp))

    def give_back(d):
        first, second = axes(d)
        part = pbuf[0, d].astype(F32)
        for k in first[1:] + second[1:]:
            arrived(r1.at[k, d], rs_r.at[d, k])
            part = part + r1[k, d].astype(F32)
        if d == 0:
            back[0] = part.astype(BF16)
        else:
            ret[d] = part.astype(BF16)
            send(ret.at[d], back.at[d], bk_s.at[d], bk_r.at[d], sp=xor(s, d, n_sp))

    slot_c = lax.broadcasted_iota(jnp.int32, (length, cap), 1).astype(F32)
    acc[...] = hidden[...]

    def combine(d):
        e = xor(s, d, n_sp)
        if d:
            arrived(back.at[d], bk_r.at[d])
        line = jnp.sum(jnp.where(expert_c == e, rank_c, 0.0), axis=1, keepdims=True)
        pick = (line == slot_c).astype(F32).astype(BF16)
        fetched = jnp.dot(pick, back[d], preferred_element_type=F32)
        weight = jnp.where(routes_c[:, 0:1] == e, rw[:, 0:1], 0.0) + jnp.where(routes_c[:, 1:2] == e, rw[:, 1:2], 0.0)
        acc[...] = acc[...] + fetched * weight

    steps = n_sp // GROUP
    stages = (gather_first, gather_second, expert, scatter_second, give_back, combine)
    for now in range(steps + len(stages) - 1):
        for behind, stage in enumerate(stages):
            step = now - behind
            if 0 <= step < steps:
                if stage is expert:
                    if step == 0:
                        for load in loads[2:]:
                            load.wait()
                    expert(step)
                else:
                    for d in range(step * GROUP, (step + 1) * GROUP):
                        stage(d)
    out[...] = acc[...].astype(out.dtype)
    for copy in sends:
        copy.wait_send()


def body(
    outer_gate, inner_gate, values, conv_taps, document, mix_proj, stream, norm_gain,
    routes, route_weight, w_gate, w_up, w_down,
):
    length, features = stream.shape
    channels = outer_gate.shape[1]
    n_sp, n_tp = lax.axis_size("sp"), lax.axis_size("tp")
    width = features // n_tp
    units = w_gate.shape[2]
    cap = -(-(3 * length // n_sp) // 16) * 16
    vmem, anywhere = pl.BlockSpec(memory_space=pltpu.VMEM), pl.BlockSpec(memory_space=pl.ANY)
    block = (n_sp, cap, width)
    dma = pltpu.SemaphoreType.DMA
    return pl.pallas_call(
        functools.partial(kernel, n_sp, n_tp, cap),
        out_shape=jax.ShapeDtypeStruct((length, width), BF16),
        in_specs=[vmem] * 9 + [anywhere] * 5,
        out_specs=vmem,
        scratch_shapes=[
            pltpu.VMEM((channels, features), BF16),
            pltpu.VMEM((length, width), BF16),
            pltpu.VMEM((features, units), BF16),
            pltpu.VMEM((features, units), BF16),
            pltpu.VMEM((units, features), BF16),
            pltpu.VMEM((16, channels), F32),
            pltpu.VMEM((16, channels), F32),
            pltpu.VMEM((length + 8, channels), F32),
            pltpu.VMEM((length + 8, channels), F32),
            pltpu.VMEM((n_tp, length, width), BF16),
            pltpu.VMEM((n_tp, length, width), BF16),
            pltpu.VMEM((length, width), F32),
            pltpu.VMEM(block, BF16),
            pltpu.VMEM((n_tp,) + block, BF16),
            pltpu.VMEM((n_tp,) + block, BF16),
            pltpu.VMEM((n_tp,) + block, BF16),
            pltpu.VMEM((GROUP * cap, units), BF16),
            pltpu.VMEM(block, BF16),
            pltpu.VMEM(block, BF16),
            pltpu.VMEM((length, width), F32),
            dma((5,)), dma, dma, dma((n_tp,)), dma((n_tp,)), dma((n_sp,)), dma((n_sp,)),
            dma((n_sp, n_tp)), dma((n_sp, n_tp)), dma((n_sp, n_tp)), dma((n_sp, n_tp)),
            dma((n_sp,)), dma((n_sp,)),
        ],
        compiler_params=pltpu.CompilerParams(
            collective_id=0, has_side_effects=True, vmem_limit_bytes=56 << 20
        ),
    )(
        outer_gate, inner_gate, values, conv_taps, document.astype(F32).reshape(-1, 1),
        routes, routes.T, route_weight, norm_gain.reshape(n_tp, width),
        mix_proj, stream, w_gate, w_up, w_down,
    )


def solution(mesh):
    return jax.shard_map(
        body,
        mesh=mesh,
        in_specs=(
            P("sp", "tp"),
            P("sp", "tp"),
            P("sp", "tp"),
            P(None, "tp"),
            P("sp"),
            P("tp", None),
            P("sp", None),
            P(),
            P("sp", None),
            P("sp", None),
            P("sp", None, "tp"),
            P("sp", None, "tp"),
            P("sp", "tp", None),
        ),
        out_specs=P("sp", "tp"),
        check_vma=False,
    )
```

```python
import functools

import jax
import jax.numpy as jnp
from jax import lax
from jax.experimental import pallas as pl
from jax.experimental.pallas import tpu as pltpu
from jax.sharding import PartitionSpec as P

F32 = jnp.float32
BF16 = jnp.bfloat16
MESH = pl.DeviceIdType.MESH
GROUP = 1
HEAD = 16


def xor(value, mask, count):
    out, bit = value, 1
    while bit < count:
        if isinstance(mask, int):
            if mask & bit:
                out = out + bit * (1 - 2 * lax.rem(lax.div(value, bit), 2))
        else:
            ours = lax.rem(lax.div(value, bit), 2)
            other = lax.rem(lax.div(mask, bit), 2)
            out = out + bit * other * (1 - 2 * ours)
        bit *= 2
    return out


def kernel(
    n_sp, n_tp, cap,
    taps, doc_r, routes_r, rw_r, gain,
    outer_hbm, inner_hbm, vals_hbm, mix_hbm, stream_hbm, wg_hbm, wu_hbm, wd_hbm,
    out,
    outer, inner, vals, mix, own, wg, wu, wd, rim_out, rim_in, prod_pad, doc_pad,
    bpart, brecv, head, hidden, obuf, xbuf, pbuf, r1, act, ret, back, acc,
    local_sem, rim_s, rim_r, br_s, br_r, hd_s, hd_r, z_s, z_r, ag_s, ag_r, rs_s, rs_r, bk_s, bk_r,
):
    s, p = lax.axis_index("sp"), lax.axis_index("tp")
    length, channels = outer.shape
    width = own.shape[1]
    features = mix.shape[1]
    hidden_units = wg.shape[1]
    x_side = 1
    while x_side * x_side < n_tp:
        x_side *= 2
    x_set = list(range(x_side))
    y_set = [k * x_side for k in range(n_tp // x_side)]

    def at(index):
        return pl.multiple_of(index * width, width)

    loads = [
        pltpu.make_async_copy(inner_hbm, inner, local_sem.at[0]),
        pltpu.make_async_copy(vals_hbm, vals, local_sem.at[1]),
        pltpu.make_async_copy(outer_hbm, outer, local_sem.at[2]),
        pltpu.make_async_copy(mix_hbm, mix, local_sem.at[3]),
        pltpu.make_async_copy(stream_hbm.at[:, pl.ds(at(p), width)], own, local_sem.at[4]),
    ]
    weight_loads = [
        pltpu.make_async_copy(wg_hbm.at[0], wg, local_sem.at[5]),
        pltpu.make_async_copy(wu_hbm.at[0], wu, local_sem.at[6]),
        pltpu.make_async_copy(wd_hbm.at[0], wd, local_sem.at[7]),
    ]
    for load in loads:
        load.start()

    barrier = pltpu.get_barrier_semaphore()
    for d in range(1, n_sp):
        pl.semaphore_signal(barrier, inc=1, device_id={"sp": xor(s, d, n_sp)}, device_id_type=MESH)
    for r in range(1, n_tp):
        pl.semaphore_signal(barrier, inc=1, device_id={"tp": xor(p, r, n_tp)}, device_id_type=MESH)
    lines = [routes_r[...].astype(F32), rw_r[...], doc_r[...].astype(F32)]
    table = jnp.concatenate(lines + [jnp.zeros((3, length), F32)], axis=0)
    table = jnp.concatenate([table] * 16, axis=0).T
    chosen = [table[:, 0:1], table[:, 1:2]]
    chosen_weight = [table[:, 2:3], table[:, 3:4]]
    docs = jnp.broadcast_to(table[:, 4:5], (length, channels))
    loads[0].wait()
    loads[1].wait()
    product = inner[...].astype(F32) * vals[...].astype(F32)
    prod_pad[8:, :] = product
    doc_pad[8:, :] = docs
    rim_out[:8, :] = product[length - 8 :]
    rim_out[8:, :] = docs[length - 8 :]
    kernel_taps = taps[...].astype(F32)

    def gated(count):
        conv = kernel_taps[2:3] * product[:count]
        for step in (1, 2):
            same = doc_pad[pl.ds(8 - step, count), :] == docs[:count]
            before = prod_pad[pl.ds(8 - step, count), :]
            conv = conv + kernel_taps[2 - step : 3 - step] * jnp.where(same, before, 0.0)
        return (outer[:count, :].astype(F32) * conv).astype(BF16)

    def branch_part(rows, r):
        lanes = pl.ds(at(xor(p, r, n_tp)), width)
        return jnp.dot(rows, mix[:, lanes], preferred_element_type=F32).astype(BF16)

    prod_pad[:8, :] = jnp.zeros((8, channels), F32)
    doc_pad[:8, :] = jnp.full((8, channels), -1.0, F32)
    loads[2].wait()
    loads[3].wait()
    rows = gated(length)
    for r in range(n_tp):
        bpart[r] = branch_part(rows, r)
    pl.semaphore_wait(barrier, n_sp - 1 + n_tp - 1)

    sends = []

    def send(src, dst, s_sem, r_sem, **device):
        copy = pltpu.make_async_remote_copy(
            src_ref=src, dst_ref=dst, send_sem=s_sem, recv_sem=r_sem,
            device_id=device, device_id_type=MESH,
        )
        copy.start()
        sends.append(copy)
        return copy

    rim = send(rim_out, rim_in, rim_s, rim_r, sp=lax.rem(s + 1, n_sp))
    for r in range(n_tp - 1, 0, -1):
        rest = pl.ds(HEAD, length - HEAD)
        send(bpart.at[r, rest], brecv.at[r, rest], br_s.at[r], br_r.at[r], tp=xor(p, r, n_tp))
    for load in weight_loads:
        load.start()

    row = lax.broadcasted_iota(jnp.int32, (length, length), 0)
    col = lax.broadcasted_iota(jnp.int32, (length, length), 1)
    expert_r = lax.broadcasted_iota(jnp.int32, (max(n_sp, 16), length), 0)
    in_r = ((routes_r[0:1, :] == expert_r) | (routes_r[1:2, :] == expert_r)).astype(F32)
    rank_r = jnp.dot(in_r.astype(BF16), (row < col).astype(F32).astype(BF16), preferred_element_type=F32)
    expert_c = lax.broadcasted_iota(jnp.int32, (length, 128), 1).astype(F32)
    in_c = ((chosen[0] == expert_c) | (chosen[1] == expert_c)).astype(F32)
    rank_c = jnp.dot((row > col).astype(F32).astype(BF16), in_c.astype(BF16), preferred_element_type=F32)
    rank_r = jnp.where(in_r > 0, rank_r, -1.0)
    rank_c = jnp.where(in_c > 0, rank_c, -1.0)

    rim.wait_recv()
    prod_pad[:8, :] = rim_in[:8, :]
    doc_pad[:8, :] = jnp.where(s > 0, rim_in[8:, :], -1.0)
    rows = gated(HEAD)
    for r in range(n_tp - 1, -1, -1):
        head[r] = branch_part(rows, r)
        if r:
            send(head.at[r], brecv.at[r, pl.ds(0, HEAD)], hd_s.at[r], hd_r.at[r], tp=xor(p, r, n_tp))
    bpart[0, :HEAD] = head[0]
    loads[4].wait()
    total = bpart[0].astype(F32)
    for r in range(1, n_tp):
        for rows, sem in ((pl.ds(HEAD, length - HEAD), br_r), (pl.ds(0, HEAD), hd_r)):
            pltpu.make_async_copy(brecv.at[r, rows], brecv.at[r, rows], sem.at[r]).wait()
        total = total + brecv[r].astype(F32)
    total = total + own[...].astype(F32)
    hidden[...] = total
    scaled = (total * gain[:, pl.ds(at(p), width)]).astype(BF16)

    slot_r = lax.broadcasted_iota(jnp.int32, (cap, length), 0).astype(F32)
    turn = [0, 2, 4, 6, 3, 5, 7, 1] + list(range(8, n_sp))
    for d in range(n_sp):
        e = xor(s, turn[d], n_sp)
        line = jnp.sum(jnp.where(expert_r == e, rank_r, 0.0), axis=0, keepdims=True)
        pick = (line == slot_r).astype(F32).astype(BF16)
        rows = jnp.dot(pick, scaled, preferred_element_type=F32).astype(BF16)
        if d == 0:
            xbuf[0, 0] = rows
        else:
            obuf[d] = rows
            send(obuf.at[d], xbuf.at[0, d], z_s.at[d], z_r.at[d], sp=e)

    def arrived(ref, sem):
        pltpu.make_async_copy(ref, ref, sem).wait()

    def axes(d):
        return (x_set, y_set) if d % 2 == 0 else (y_set, x_set)

    def gather_first(d):
        first, _ = axes(d)
        if d:
            arrived(xbuf.at[0, d], z_r.at[d])
        for f in first[1:]:
            send(xbuf.at[0, d], xbuf.at[f, d], ag_s.at[d, f], ag_r.at[d, f], tp=xor(p, f, n_tp))

    def gather_second(d):
        first, second = axes(d)
        for f in first:
            if f:
                arrived(xbuf.at[f, d], ag_r.at[d, f])
            for g in second[1:]:
                send(
                    xbuf.at[f, d], xbuf.at[f + g, d], ag_s.at[d, f + g], ag_r.at[d, f + g],
                    tp=xor(p, g, n_tp),
                )

    tile = min(256, hidden_units)

    def expert_up(low):
        for d in range(low, low + GROUP):
            first, second = axes(d)
            for f in first:
                for g in second[1:]:
                    arrived(xbuf.at[f + g, d], ag_r.at[d, f + g])
        square = jnp.zeros((GROUP * cap, 1), F32)
        for r in range(n_tp):
            inverse = 1.0 / gain[:, pl.ds(at(xor(p, r, n_tp)), width)]
            plain = xbuf[r, low : low + GROUP].reshape(GROUP * cap, width).astype(F32) * inverse
            square = square + jnp.sum(plain * plain, axis=1, keepdims=True)
        scale = lax.rsqrt(square / features + 1e-06)

        def up_tile(j, _):
            lanes = pl.ds(pl.multiple_of(j * tile, tile), tile)
            gate = jnp.zeros((GROUP * cap, tile), F32)
            upper = jnp.zeros((GROUP * cap, tile), F32)
            for r in range(n_tp):
                lhs = xbuf[r, low : low + GROUP].reshape(GROUP * cap, width)
                deep = pl.ds(at(xor(p, r, n_tp)), width)
                gate = gate + jnp.dot(lhs, wg[deep, lanes], preferred_element_type=F32)
                upper = upper + jnp.dot(lhs, wu[deep, lanes], preferred_element_type=F32)
            gate, upper = gate * scale, upper * scale
            act[:, lanes] = (gate / (1.0 + jnp.exp(-gate)) * upper).astype(BF16)
            return 0

        lax.fori_loop(0, hidden_units // tile, up_tile, 0)

    def expert_down(low):
        for r in range(n_tp - 1, -1, -1):
            lanes = pl.ds(at(xor(p, r, n_tp)), width)
            part = jnp.dot(act[...], wd[:, lanes], preferred_element_type=F32).astype(BF16)
            pbuf[r, low : low + GROUP] = part.reshape(GROUP, cap, width)
            for d in range(low, low + GROUP):
                first, second = axes(d)
                for f in first[1:]:
                    if r - f in second:
                        send(
                            pbuf.at[r, d], r1.at[r, d], rs_s.at[d, r], rs_r.at[d, r],
                            tp=xor(p, f, n_tp),
                        )

    def scatter_second(d):
        first, second = axes(d)
        for g in second[1:]:
            part = pbuf[g, d].astype(F32)
            for f in first[1:]:
                arrived(r1.at[f + g, d], rs_r.at[d, f + g])
                part = part + r1[f + g, d].astype(F32)
            pbuf[g, d] = part.astype(BF16)
            send(pbuf.at[g, d], r1.at[g, d], rs_s.at[d, g], rs_r.at[d, g], tp=xor(p, g, n_tp))

    def give_back(d):
        first, second = axes(d)
        part = pbuf[0, d].astype(F32)
        for k in first[1:] + second[1:]:
            arrived(r1.at[k, d], rs_r.at[d, k])
            part = part + r1[k, d].astype(F32)
        if d == 0:
            back[0] = part.astype(BF16)
        else:
            ret[d] = part.astype(BF16)
            send(ret.at[d], back.at[d], bk_s.at[d], bk_r.at[d], sp=xor(s, turn[d], n_sp))

    slot_c = lax.broadcasted_iota(jnp.int32, (length, cap), 1).astype(F32)
    acc[...] = hidden[...]

    def combine(d):
        e = xor(s, turn[d], n_sp)
        if d:
            arrived(back.at[d], bk_r.at[d])
        line = jnp.sum(jnp.where(expert_c == e.astype(F32), rank_c, 0.0), axis=1, keepdims=True)
        pick = (line == slot_c).astype(F32).astype(BF16)
        fetched = jnp.dot(pick, back[d], preferred_element_type=F32)
        weight = sum(jnp.where(c == e.astype(F32), w, 0.0) for c, w in zip(chosen, chosen_weight))
        acc[...] = acc[...] + fetched * weight

    def run(stage, *steps):
        for step in steps:
            if 0 <= step < count:
                low = step * GROUP
                if stage in (expert_up, expert_down):
                    stage(low)
                else:
                    for d in range(low, low + GROUP):
                        stage(d)

    count = n_sp // GROUP
    run(gather_first, 0)
    run(gather_first, 1)
    run(gather_second, 0)
    run(gather_first, 2)
    run(gather_second, 1)
    run(gather_first, 3)
    run(gather_second, 2)
    for load in weight_loads:
        load.wait()
    for step in range(count + 8):
        run(expert_up, step + 0)
        run(gather_first, step + 4)
        run(gather_second, step + 3)
        run(expert_down, step + 0)
        run(scatter_second, step - 2)
        run(give_back, step - 4)
        run(combine, step - 6)
    out[...] = acc[...].astype(out.dtype)
    for copy in sends:
        copy.wait_send()


def body(
    outer_gate, inner_gate, values, conv_taps, document, mix_proj, stream, norm_gain,
    routes, route_weight, w_gate, w_up, w_down,
):
    length, features = stream.shape
    channels = outer_gate.shape[1]
    n_sp, n_tp = lax.axis_size("sp"), lax.axis_size("tp")
    width = features // n_tp
    units = w_gate.shape[2]
    cap = -(-(3 * length // n_sp) // 16) * 16
    vmem, anywhere = pl.BlockSpec(memory_space=pltpu.VMEM), pl.BlockSpec(memory_space=pl.ANY)
    block = (n_sp, cap, width)
    dma = pltpu.SemaphoreType.DMA
    return pl.pallas_call(
        functools.partial(kernel, n_sp, n_tp, cap),
        out_shape=jax.ShapeDtypeStruct((length, width), BF16),
        in_specs=[vmem] * 5 + [anywhere] * 8,
        out_specs=vmem,
        scratch_shapes=[
            pltpu.VMEM((length, channels), BF16),
            pltpu.VMEM((length, channels), BF16),
            pltpu.VMEM((length, channels), BF16),
            pltpu.VMEM((channels, features), BF16),
            pltpu.VMEM((length, width), BF16),
            pltpu.VMEM((features, units), BF16),
            pltpu.VMEM((features, units), BF16),
            pltpu.VMEM((units, features), BF16),
            pltpu.VMEM((16, channels), F32),
            pltpu.VMEM((16, channels), F32),
            pltpu.VMEM((length + 8, channels), F32),
            pltpu.VMEM((length + 8, channels), F32),
            pltpu.VMEM((n_tp, length, width), BF16),
            pltpu.VMEM((n_tp, length, width), BF16),
            pltpu.VMEM((n_tp, HEAD, width), BF16),
            pltpu.VMEM((length, width), F32),
            pltpu.VMEM(block, BF16),
            pltpu.VMEM((n_tp,) + block, BF16),
            pltpu.VMEM((n_tp,) + block, BF16),
            pltpu.VMEM((n_tp,) + block, BF16),
            pltpu.VMEM((GROUP * cap, units), BF16),
            pltpu.VMEM(block, BF16),
            pltpu.VMEM(block, BF16),
            pltpu.VMEM((length, width), F32),
            dma((8,)), dma, dma, dma((n_tp,)), dma((n_tp,)), dma((n_tp,)), dma((n_tp,)), dma((n_sp,)), dma((n_sp,)),
            dma((n_sp, n_tp)), dma((n_sp, n_tp)), dma((n_sp, n_tp)), dma((n_sp, n_tp)),
            dma((n_sp,)), dma((n_sp,)),
        ],
        compiler_params=pltpu.CompilerParams(
            collective_id=0, has_side_effects=True, vmem_limit_bytes=56 << 20
        ),
    )(
        conv_taps, document.reshape(1, -1), routes.T, route_weight.T, norm_gain.reshape(1, -1),
        outer_gate, inner_gate, values, mix_proj, stream, w_gate, w_up, w_down,
    )


def solution(mesh):
    return jax.shard_map(
        body,
        mesh=mesh,
        in_specs=(
            P("sp", "tp"),
            P("sp", "tp"),
            P("sp", "tp"),
            P(None, "tp"),
            P("sp"),
            P("tp", None),
            P("sp", None),
            P(),
            P("sp", None),
            P("sp", None),
            P("sp", None, "tp"),
            P("sp", None, "tp"),
            P("sp", "tp", None),
        ),
        out_specs=P("sp", "tp"),
        check_vma=False,
    )
```
